128 devices in a mesh: ep: 64 (over z, y, x), tp: 2 (over core).
Axes of the slice: x: 4, y: 4, z: 4, core: 2. Of those that a mesh axis runs over, the one named last changes fastest.
Arguments:
- inputs: bfloat16 [1024, 2048], P('ep'), may hold values from -6 to 6
- positions: int32 [1024], P('ep'), may hold values from 1024 to 8191
- ret_state: float32 [1024, 12, 128, 128], P('ep', 'tp'), may hold values from -4 to 4
- norm_mix: bfloat16 [2048], replicated, may hold values from 0.099609375 to 1.8984375
- w_query: bfloat16 [2048, 1536], P('ep', 'tp'), may hold values from -0.375 to 0.375
- w_key: bfloat16 [2048, 1536], P('ep', 'tp'), may hold values from -0.375 to 0.375
- w_value: bfloat16 [2048, 1536], P('ep', 'tp'), may hold values from -0.375 to 0.375
- w_gate_in: bfloat16 [2048, 1536], P('ep', 'tp'), may hold values from -0.375 to 0.375
- head_gain: bfloat16 [1536], P('tp'), may hold values from 0.099609375 to 1.8984375
- w_out: bfloat16 [1536, 2048], P('tp', 'ep'), may hold values from -0.15625 to 0.15625
- norm_ffn: bfloat16 [2048], replicated, may hold values from 0.099609375 to 1.8984375
- route_ids: int32 [1024, 4], P('ep'), may hold values from 0 to 63, all different within a row; in each aligned block of 16 rows (0 to 15, 16 to 31, ...) at most 2 rows name the same one
- route_weight: bfloat16 [1024, 4], P('ep'), may hold values from 0.19921875 to 1
- exp_gate: bfloat16 [64, 2048, 1024], P('ep', None, 'tp'), may hold values from -0.125 to 0.125
- exp_up: bfloat16 [64, 2048, 1024], P('ep', None, 'tp'), may hold values from -0.125 to 0.125
- exp_down: bfloat16 [64, 1024, 2048], P('ep', 'tp'), may hold values from -0.1875 to 0.1875
- dense_gate: bfloat16 [2048, 4096], P(None, ('ep', 'tp')), may hold values from -0.125 to 0.125
- dense_up: bfloat16 [2048, 4096], P(None, ('ep', 'tp')), may hold values from -0.125 to 0.125
- dense_down: bfloat16 [4096, 2048], P(('ep', 'tp')), may hold values from -0.375 to 0.375
- branch_gate: bfloat16 [2048], replicated, may hold values from -0.125 to 0.125
Outputs:
- layer_out: bfloat16 [1024, 2048], P('ep')
- new_state: float32 [1024, 12, 128, 128], P('ep', 'tp')
The draws below stay inside these ranges and needn't reach their ends.
Inputs may be any that keep to these rules, and one draw needn't show every extreme that they name: `route_ids`: each row names 4 different experts. Among the rows of one index of ep no expert is named more than 2 times, a bound that some block reaches.
All inputs are finite; a program needn't handle non-finite values.
Results may differ from the reference program's by a relative error of at most 0.015.
Values may be sent and summed in bfloat16 or wider, within the bound.
A program may use at most 128 MiB of HBM per device.

```python
import math
from functools import reduce
import jax
import jax.numpy as jnp
import numpy as np
from jax import lax

D = 2048
HEADS = 12
HEAD_DIM = 128
EXP_FF = 1024
DENSE_FF = 4096
TOP_K = 4
SEQ_DEV = 16
RET_WIDTH = 1536
EXPERTS = 64
TOKENS = 1024
CAP = 2
N_EP = 64
N_TP = 2


def place_ends(drawn, stream_key, smallest, top_value):
    index_at = [jax.random.randint(jax.random.fold_in(stream_key, axis), (), 0, length) for axis, length in enumerate(drawn.shape)]
    longest = drawn.shape.index(max(drawn.shape))
    next_to = index_at[:longest] + [(index_at[longest] + 1) % drawn.shape[longest]] + index_at[longest + 1:]
    return drawn.at[tuple(index_at)].set(smallest).at[tuple(next_to)].set(top_value)


def raised(values, own_key, source, target, blocks, factor):
    def block_of(position):
        return (jnp.arange(values.shape[position]) // (values.shape[position] // blocks)).reshape((-1,) + (1,) * (values.ndim - 1 - position))

    first = jax.random.permutation(own_key, blocks)[block_of(target)]
    far = (block_of(target) + blocks // 2) % blocks
    return jnp.where((block_of(source) == first) | (block_of(source) == far), factor * values, values)


def block_scale(key, shape, shards, smallest, top_value):
    def one(axis_at, parts):
        draws = jax.random.uniform(jax.random.fold_in(jax.random.fold_in(key, 6), axis_at), (parts,), jnp.float32, smallest / len(shards), top_value / len(shards))
        return jnp.repeat(jnp.exp(draws), shape[axis_at] // parts).reshape((-1,) + (1,) * (len(shape) - axis_at - 1))

    loudness = one(*shards[0])
    for cut in shards[1:]:
        loudness = loudness * one(*cut)
    return loudness


def deal_out(rng, own, number, rows, amount, top, reach, lean):
    order = jax.random.permutation(rng, amount)
    heavy_load, ordinary = load_shares(amount, rows * top, reach, lean, True), load_shares(amount, rows * top, reach, lean, False)
    places = jnp.arange(amount)

    def named(lengths, turn):
        used = int((lengths > 0).sum())
        fixed = max(1, used // 4)
        moved = fixed + (places - fixed + turn * (used - fixed)) % max(1, amount - fixed)
        return jnp.zeros((amount,), jnp.int32).at[order[jnp.where(places < fixed, places, moved)]].set(jnp.asarray(lengths, jnp.int32))

    lengths = jnp.where(number % 4 == 0, named(heavy_load, number // 4), named(ordinary, number - number // 4 - 1))
    mixed = jax.random.permutation(jax.random.fold_in(own, 3), amount)
    giver, receiver = mixed[0:amount // 2 * 2:2], mixed[1:amount // 2 * 2:2]
    margin = jnp.minimum(lengths[giver] - 1, reach - lengths[receiver]) // 2
    margin = jnp.where((giver == order[0]) | (receiver == order[0]) | (lengths[receiver] == 0), 0, jnp.maximum(margin, 0))
    moved = jax.random.randint(jax.random.fold_in(own, 4), (amount // 2,), 0, 1 << 20) % (margin + 1)
    lengths = lengths.at[giver].add(-moved).at[receiver].add(moved)
    items = jnp.searchsorted(jnp.cumsum(lengths), jnp.arange(rows * top), side="right").astype(jnp.int32)
    grid = items.reshape(top, rows).T
    grid = grid[jax.random.permutation(jax.random.fold_in(own, 1), rows)]
    turn = jax.random.randint(jax.random.fold_in(own, 2), (rows, 1), 0, top)
    return jnp.take_along_axis(grid, (jnp.arange(top)[None, :] + turn) % top, axis=1)


def load_shares(amount, total, bound, slope, full):
    portions = [(1 << 20) // math.isqrt(standing ** slope) + 1 for standing in range(1, amount + 1)]
    largest = bound if full else min(bound, max(-(-total // amount), total * portions[0] // sum(portions)))
    least = 1 if total - largest >= amount - 1 else 0
    given, rest = [largest] + [least] * (amount - 1), total - largest - least * (amount - 1)
    while rest > 0:
        candidates = [i for i in range(1, amount) if given[i] < largest] or [i for i in range(1, amount) if given[i] < bound]
        pool, budget = sum([portions[i] for i in candidates]), rest
        for i in candidates:
            addition = min(bound - given[i], max(1, budget * portions[i] // pool), rest)
            given[i] = given[i] + addition
            rest = rest - addition
    return np.array(given)


def scatter_about(stream_key, dims, scale, bound, pieces=(), kind=jnp.bfloat16):
    drawn = jax.random.normal(stream_key, dims, jnp.float32) * scale
    if len(pieces) > 0:
        drawn = block_scale(stream_key, dims, pieces, -0.22, 0.18) * drawn
    return jnp.clip(drawn, min=-bound, max=bound).astype(kind)


def gaussian_with(key, dims, deviation, reach, shards, heavy, kind=jnp.bfloat16):
    values = deviation * jax.random.normal(key, dims, jnp.float32)
    if shards:
        values = values * block_scale(key, dims, shards, -0.22, 0.18)
    return jnp.clip(raised(values, jax.random.fold_in(key, 3), *heavy), -reach, reach).astype(kind)


def setup_inputs(seed: int = 0) -> dict:
    keys = jax.random.split(jax.random.key(seed), 21)
    inputs = scatter_about(keys[0], (TOKENS, D), 1.0, 6.0, ((0, 64),))
    positions = place_ends(jax.random.randint(keys[1], (TOKENS,), 1024, 8192), jax.random.fold_in(keys[1], 1), 1024, 8191).astype(jnp.int32)
    ret_state = scatter_about(keys[2], (TOKENS, HEADS, HEAD_DIM, HEAD_DIM), 0.25, 4.0, ((0, 64), (1, 2)), jnp.float32)
    norm_mix = jnp.clip(1.0 + 0.18 * jax.random.normal(keys[3], (D,), jnp.float32), 0.099609375, 1.8984375).astype(jnp.bfloat16)
    w_query = gaussian_with(keys[4], (D, RET_WIDTH), D ** -0.5, 0.375, ((0, 64), (1, 2)), (0, 1, 64, 4.0))
    w_key = gaussian_with(keys[5], (D, RET_WIDTH), D ** -0.5, 0.375, ((0, 64), (1, 2)), (0, 1, 64, 4.0))
    w_value = gaussian_with(keys[6], (D, RET_WIDTH), D ** -0.5, 0.375, ((0, 64), (1, 2)), (0, 1, 64, 4.0))
    w_gate_in = gaussian_with(keys[7], (D, RET_WIDTH), D ** -0.5, 0.375, ((0, 64), (1, 2)), (0, 1, 64, 4.0))
    head_gain = jnp.clip(1.0 + 0.18 * jax.random.normal(keys[8], (RET_WIDTH,), jnp.float32), 0.099609375, 1.8984375).astype(jnp.bfloat16)
    w_out = scatter_about(keys[9], (RET_WIDTH, D), RET_WIDTH ** -0.5, 0.15625, ((0, 2), (1, 64)))
    norm_ffn = jnp.clip(1.0 + 0.18 * jax.random.normal(keys[10], (D,), jnp.float32), 0.099609375, 1.8984375).astype(jnp.bfloat16)
    route_ids_keys = jax.random.split(jax.random.fold_in(keys[11], 1), TOKENS // SEQ_DEV)
    route_ids_turns = jax.random.permutation(jax.random.fold_in(keys[11], 3), TOKENS // SEQ_DEV)
    route_ids = jax.vmap(lambda own, number: deal_out(jax.random.fold_in(keys[11], 2), own, number, SEQ_DEV, EXPERTS, TOP_K, CAP, 2))(route_ids_keys, route_ids_turns).reshape((TOKENS, TOP_K))
    route_weight = jnp.clip(jnp.exp(math.log(1.0) - 1.6133518 * jax.random.uniform(keys[12], (TOKENS, TOP_K), jnp.float32) ** block_scale(keys[12], (TOKENS, TOP_K), ((0, 64),), -0.2, 0.2)), 0.19921875, 1.0).astype(jnp.bfloat16)
    exp_gate = scatter_about(keys[13], (EXPERTS, D, EXP_FF), D ** -0.5, 0.125, ((0, 64), (2, 2)))
    exp_up = scatter_about(keys[14], (EXPERTS, D, EXP_FF), D ** -0.5, 0.125, ((0, 64), (2, 2)))
    exp_down = scatter_about(keys[15], (EXPERTS, EXP_FF, D), EXP_FF ** -0.5, 0.1875, ((0, 64), (1, 2)))
    dense_gate = scatter_about(keys[16], (D, DENSE_FF), D ** -0.5, 0.125, ((1, 128),))
    dense_up = scatter_about(keys[17], (D, DENSE_FF), D ** -0.5, 0.125, ((1, 128),))
    dense_down = gaussian_with(keys[18], (DENSE_FF, D), DENSE_FF ** -0.5, 0.375, ((0, 128),), (0, 1, 128, 5.5))
    branch_gate = scatter_about(keys[19], (D,), D ** -0.5, 0.125)
    return {"inputs": inputs, "positions": positions, "ret_state": ret_state, "norm_mix": norm_mix, "w_query": w_query, "w_key": w_key, "w_value": w_value, "w_gate_in": w_gate_in, "head_gain": head_gain, "w_out": w_out, "norm_ffn": norm_ffn, "route_ids": route_ids, "route_weight": route_weight, "exp_gate": exp_gate, "exp_up": exp_up, "exp_down": exp_down, "dense_gate": dense_gate, "dense_up": dense_up, "dense_down": dense_down, "branch_gate": branch_gate}


EPS = 1e-06

def rms_scale(values, scales):
    widened = values.astype(jnp.float32)
    scaled = widened * lax.rsqrt(lax.optimization_barrier(jnp.mean(widened * widened, axis=-1, keepdims=True)) + EPS)
    return (scaled * scales.astype(jnp.float32)).astype(jnp.bfloat16)

def rotary_angles(positions, head_dim):
    halfway = head_dim // 2
    frequency = 10000.0 ** (-jnp.arange(halfway, dtype=jnp.float32) * 2.0 / head_dim)
    return positions.astype(jnp.float32)[:, None] * frequency[None, :]

def rotate_heads(values, angles):
    halfway = values.shape[-1] // 2
    cosine = jnp.cos(angles)[:, None, :]
    sine_of = jnp.sin(angles)[:, None, :]
    leading = values[..., :halfway]
    trailing = values[..., halfway:]
    return jnp.concatenate([leading * cosine - trailing * sine_of, trailing * cosine + leading * sine_of], axis=-1)

def log_decay(head_count):
    spread = jnp.arange(head_count, dtype=jnp.float32) * (5.0 / max(head_count - 1, 1))
    return jnp.log1p(-2.0 ** (-5.0 - spread))

def retain(queries, keys_in, values_in, gate_pre, old_state, positions, scales, log_gamma):
    row_count, head_count, head_dim = (old_state.shape[0], old_state.shape[1], old_state.shape[2])
    angles = rotary_angles(positions, head_dim)
    rot_query = rotate_heads(queries.astype(jnp.float32).reshape(row_count, head_count, head_dim), angles)
    rot_key = rotate_heads(keys_in.astype(jnp.float32).reshape(row_count, head_count, head_dim), angles) * head_dim ** (-0.5)
    value_heads = values_in.astype(jnp.float32).reshape(row_count, head_count, head_dim)
    new_state = jnp.exp(log_gamma)[None, :, None, None] * old_state + rot_key[:, :, :, None] * value_heads[:, :, None, :]
    readout = jnp.einsum('shd,shdv->shv', rot_query, new_state, precision=lax.Precision.HIGHEST)
    centred = readout - lax.optimization_barrier(jnp.mean(readout, axis=-1, keepdims=True))
    normed = centred * lax.rsqrt(lax.optimization_barrier(jnp.mean(centred * centred, axis=-1, keepdims=True)) + EPS)
    normed = normed * scales.astype(jnp.float32).reshape(head_count, head_dim)
    gated_out = normed.reshape(row_count, head_count * head_dim) * jax.nn.silu(gate_pre.astype(jnp.float32))
    return (gated_out.astype(jnp.bfloat16), new_state)

def expert_total(normed_ffn, route_ids, route_share, exp_gate, exp_up, exp_down):
    token_count = normed_ffn.shape[0]
    flat_ids = route_ids.reshape(-1)
    flat_share = route_share.reshape(-1)
    most_rows = N_EP * CAP

    def one_expert(running, expert):
        matches = flat_ids == expert
        where_hit = jnp.nonzero(matches, size=most_rows, fill_value=0)[0].astype(jnp.int32)
        in_use = jnp.arange(most_rows, dtype=jnp.int32) < jnp.sum(matches.astype(jnp.int32))
        token_of = (where_hit // TOP_K).astype(jnp.int32)
        chosen = normed_ffn[token_of]
        gate_part = jnp.dot(chosen, exp_gate[expert], preferred_element_type=jnp.float32)
        up_part = jnp.dot(chosen, exp_up[expert], preferred_element_type=jnp.float32)
        hidden = (jax.nn.silu(gate_part) * up_part).astype(jnp.bfloat16)
        result = jnp.dot(hidden, exp_down[expert], preferred_element_type=jnp.float32)
        picked = flat_share[where_hit]
        weight = jnp.where(in_use, picked, jnp.zeros_like(picked))
        return (running.at[token_of].add(result * weight[:, None]), None)
    running, _ = lax.scan(one_expert, jnp.zeros((token_count, D), jnp.float32), jnp.arange(EXPERTS, dtype=jnp.int32))
    return running

def reference(inputs, positions, ret_state, norm_mix, w_query, w_key, w_value, w_gate_in, head_gain, w_out, norm_ffn, route_ids, route_weight, exp_gate, exp_up, exp_down, dense_gate, dense_up, dense_down, branch_gate):
    normed = rms_scale(inputs, norm_mix)
    queries = jnp.dot(normed, w_query, preferred_element_type=jnp.float32).astype(jnp.bfloat16)
    keys_new = jnp.dot(normed, w_key, preferred_element_type=jnp.float32).astype(jnp.bfloat16)
    values_new = jnp.dot(normed, w_value, preferred_element_type=jnp.float32).astype(jnp.bfloat16)
    gate_pre = jnp.dot(normed, w_gate_in, preferred_element_type=jnp.float32).astype(jnp.bfloat16)
    retained, new_state = retain(queries, keys_new, values_new, gate_pre, ret_state, positions, head_gain, log_decay(HEADS))
    group_width = RET_WIDTH // N_TP
    halves = [lax.optimization_barrier(jnp.dot(retained[:, member * group_width:(member + 1) * group_width], w_out[member * group_width:(member + 1) * group_width], preferred_element_type=jnp.float32).astype(jnp.bfloat16)).astype(jnp.float32) for member in range(N_TP)]
    mixer_out = reduce(jnp.add, halves).astype(jnp.bfloat16)
    residual_sum = (inputs.astype(jnp.float32) + mixer_out.astype(jnp.float32)).astype(jnp.bfloat16)
    normed_ffn = rms_scale(residual_sum, norm_ffn)
    dense_hidden = (jax.nn.silu(jnp.dot(normed_ffn, dense_gate, preferred_element_type=jnp.float32)) * jnp.dot(normed_ffn, dense_up, preferred_element_type=jnp.float32)).astype(jnp.bfloat16)
    dense_result = jnp.dot(dense_hidden, dense_down, preferred_element_type=jnp.float32)
    branch_open = jax.nn.sigmoid(jnp.dot(normed_ffn, branch_gate[:, None], preferred_element_type=jnp.float32))
    widened = route_weight.astype(jnp.float32)
    route_share = widened / lax.optimization_barrier(jnp.sum(widened, axis=-1, keepdims=True))
    experts_out = expert_total(normed_ffn, route_ids, route_share, exp_gate, exp_up, exp_down)
    layer_out = (residual_sum.astype(jnp.float32) + experts_out + branch_open * dense_result).astype(jnp.bfloat16)
    return (layer_out, new_state)
```

```python
import functools

import jax
import jax.numpy as jnp
from jax import lax
from jax.experimental import pallas as pl
from jax.experimental.pallas import tpu as pltpu
from jax.sharding import PartitionSpec as P

D = 2048
HEADS = 12
HD = 128
LH = 6
RW = 768
T = 16
NZ = 4
NP = 16
EPS = 1e-06
MESH = pl.DeviceIdType.MESH
F32 = jnp.float32
BF16 = jnp.bfloat16
NT = (((1,), (1,)), ((), ()))
ANY = pl.BlockSpec(memory_space=pl.ANY)
VM = pl.BlockSpec(memory_space=pltpu.VMEM)
SM = pl.BlockSpec(memory_space=pltpu.SMEM)


class Links:
    def __init__(self, send, recv, local):
        ep = lax.axis_index("ep")
        self.c = lax.axis_index("tp")
        self.z = ep // NP
        self.p = ep % NP
        self.y = self.p // 4
        self.x = self.p % 4
        self.send, self.recv, self.local = send, recv, local
        self.n = 0
        self.m = 0

    def plane(self, d):
        return ((self.y + d // 4) % 4) * 4 + (self.x + d % 4) % 4

    def chip(self, z, p):
        return z * NP + p

    def push(self, src, dst, ep, tp):
        k = self.n
        self.n += 1
        copy = pltpu.make_async_remote_copy(
            src_ref=src,
            dst_ref=dst,
            send_sem=self.send.at[k],
            recv_sem=self.recv.at[k],
            device_id=(ep, tp),
            device_id_type=MESH,
        )
        copy.start()
        return copy

    def pull(self, src, dst):
        k = self.m
        self.m += 1
        copy = pltpu.make_async_copy(src, dst, self.local.at[k])
        copy.start()
        return copy

    def barrier_signal(self, both_cores):
        bar = pltpu.get_barrier_semaphore()
        peers = [(self.chip(self.z, self.plane(d)), self.c) for d in range(1, NP)]
        peers += [(self.chip((self.z + k) % NZ, self.p), self.c) for k in range(1, NZ)]
        if both_cores:
            peers += [(self.chip((self.z + k) % NZ, self.p), 1 - self.c) for k in range(NZ)]
        for peer in peers:
            pl.semaphore_signal(bar, inc=1, device_id=peer, device_id_type=MESH)
        return bar, len(peers)


def rms(values, scales):
    scaled = values * lax.rsqrt(jnp.mean(values * values, axis=-1, keepdims=True) + EPS)
    return (scaled * scales.astype(F32)).astype(BF16)


def project_kernel(
    x_ref, gain_ref, wq, wk, wv, wg, wo_in, dg_in, du_in, dd_in,
    q_ref, wo_out, dw_out,
    xs, xg, wz, wo_own, d_own, part, rsl, send, recv, local,
):
    at = Links(send, recv, local)
    z, p, c = at.z, at.p, at.c
    bar, greeted = at.barrier_signal(False)
    w_copies = [
        at.pull(w, wz.at[z, :, j * RW : (j + 1) * RW]) for j, w in enumerate((wq, wk, wv, wg))
    ]
    wo_copy = at.pull(wo_in, wo_own)
    d_copies = [at.pull(w, d_own.at[j]) for j, w in enumerate((dg_in, du_in, dd_in))]
    n = rms(x_ref[...].astype(F32), gain_ref[...]).astype(F32)
    lane_block = lax.broadcasted_iota(jnp.int32, (T, 128), 1) // 32
    for y in range(4):
        for x in range(4):
            piece = jnp.zeros((T, 128), F32)
            for k in range(NZ):
                tile = n[:, k * 512 + y * 128 : k * 512 + (y + 1) * 128]
                turn = ((k - x) * 32) % 128
                if turn:
                    tile = pltpu.roll(tile, turn, 1)
                piece = jnp.where(lane_block == k, tile, piece)
            xs[y * 4 + x] = piece.astype(BF16)
    xg[0] = xs[p]
    pl.semaphore_wait(bar, greeted)
    up, down = (z + 1) % NZ, (z + 3) % NZ
    for copy in w_copies:
        copy.wait()
    w_up = at.push(wz.at[z], wz.at[z], at.chip(up, p), c)
    w_down = at.push(wz.at[z], wz.at[z], at.chip(down, p), c)
    x_sends = []
    for d in range(1, NP):
        q = at.plane(d)
        x_sends.append(at.push(xs.at[q], xg.at[d], at.chip(z, q), c))
    wo_copy.wait()
    wo_keep = at.pull(wo_own, wo_out.at[p])
    wo_sends = []
    for d in range(1, NP):
        q = at.plane(d)
        wo_sends.append(at.push(wo_own, wo_out.at[p], at.chip(z, q), c))
    half = 2 * RW
    w_up.wait_recv()
    w_up2 = at.push(wz.at[down, :, :half], wz.at[down, :, :half], at.chip(up, p), c)
    w_down.wait_recv()
    w_down2 = at.push(wz.at[up, :, half:], wz.at[up, :, half:], at.chip(down, p), c)
    for copy in d_copies:
        copy.wait()
    d_keep = at.pull(d_own, dw_out.at[z])
    d_up = at.push(d_own, dw_out.at[z], at.chip(up, p), c)
    d_down = at.push(d_own, dw_out.at[z], at.chip(down, p), c)
    for copy in x_sends:
        copy.wait_recv()
    w_up2.wait_recv()
    w_down2.wait_recv()
    rows = xg[...].reshape(NP * T, 128)
    for j in range(4):
        cols = slice(j * RW, (j + 1) * RW)
        w = wz[:, :, cols].reshape(128, RW)
        prod = jnp.dot(rows, w, preferred_element_type=F32)
        part[:, :, cols] = prod.astype(BF16).reshape(NP, T, RW)
    r_sends = []
    for d in range(1, NP):
        back = (((at.y + 4 - d // 4) % 4) * 4) + (at.x + 4 - d % 4) % 4
        r_sends.append(at.push(part.at[d], rsl.at[d], at.chip(z, back), c))
    d_up.wait_recv()
    d_up2 = at.push(
        dw_out.at[down, :, :, :1024], dw_out.at[down, :, :, :1024], at.chip(up, p), c
    )
    d_down.wait_recv()
    d_down2 = at.push(dw_out.at[up, :, :, 1024:], dw_out.at[up, :, :, 1024:], at.chip(down, p), c)
    total = part[0].astype(F32)
    for d in range(1, NP):
        r_sends[d - 1].wait_recv()
        total = total + rsl[d].astype(F32)
    q_ref[...] = total.astype(BF16)
    for copy in wo_sends + [d_up2, d_down2]:
        copy.wait_recv()
    for copy in [w_up, w_down, w_up2, w_down2, d_up, d_down, d_up2, d_down2]:
        copy.wait_send()
    for copy in x_sends + wo_sends + r_sends:
        copy.wait_send()
    wo_keep.wait()
    d_keep.wait()


def project(x, gain, wq, wk, wv, wg, wo_t, dg_t, du_t, dd):
    return pl.pallas_call(
        project_kernel,
        out_shape=(
            jax.ShapeDtypeStruct((T, 4 * RW), BF16),
            jax.ShapeDtypeStruct((NP, 32, RW), BF16),
            jax.ShapeDtypeStruct((NZ, 3, 32, D), BF16),
        ),
        in_specs=[VM, VM] + [ANY] * 8,
        out_specs=(VM, ANY, ANY),
        scratch_shapes=[
            pltpu.VMEM((NP, T, 128), BF16),
            pltpu.VMEM((NP, T, 128), BF16),
            pltpu.VMEM((NZ, 32, 4 * RW), BF16),
            pltpu.VMEM((32, RW), BF16),
            pltpu.VMEM((3, 32, D), BF16),
            pltpu.VMEM((NP, T, 4 * RW), BF16),
            pltpu.VMEM((NP, T, 4 * RW), BF16),
            pltpu.SemaphoreType.DMA((56,)),
            pltpu.SemaphoreType.DMA((56,)),
            pltpu.SemaphoreType.DMA((12,)),
        ],
        compiler_params=pltpu.CompilerParams(collective_id=0, has_side_effects=True),
        name="project",
    )(x, gain, wq, wk, wv, wg, wo_t, dg_t, du_t, dd)


STEP = 2


def state_kernel(q_ref, cos_ref, sin_ref, gain_ref, gamma_ref, s_ref, ret_ref, new_ref, qk, vv, ro):
    i = pl.program_id(0)

    @pl.when(i == 0)
    def _():
        cosine, sine = cos_ref[...], sin_ref[...]
        for h in range(LH):
            for part, row, scale in ((0, 0, None), (1, 8, HD**-0.5)):
                f = q_ref[:, part * RW + h * HD : part * RW + (h + 1) * HD].astype(F32)
                turned = f * cosine + pltpu.roll(f, 64, 1) * sine
                if scale is not None:
                    turned = turned * scale
                qk[:, row + h, :] = turned
            vv[:, h, :] = q_ref[:, 2 * RW + h * HD : 2 * RW + (h + 1) * HD].astype(F32)

    for t in range(STEP):
        tok = i * STEP + t
        columns = qk[tok].T
        v = vv[tok]
        for h in range(LH):
            new = gamma_ref[h] * s_ref[t, h] + columns[:, 8 + h : 9 + h] * v[h : h + 1, :]
            new_ref[t, h] = new
            ro[tok, h : h + 1, :] = jnp.sum(columns[:, h : h + 1] * new, axis=0, keepdims=True)

    @pl.when(i == pl.num_programs(0) - 1)
    def _():
        for h in range(LH):
            cols = slice(h * HD, (h + 1) * HD)
            r = ro[:, h, :]
            centred = r - jnp.mean(r, axis=-1, keepdims=True)
            normed = centred * lax.rsqrt(jnp.mean(centred * centred, axis=-1, keepdims=True) + EPS)
            normed = normed * gain_ref[:, cols].astype(F32)
            gate = q_ref[:, 3 * RW + h * HD : 3 * RW + (h + 1) * HD].astype(F32)
            ret_ref[:, cols] = (normed * (gate * jax.nn.sigmoid(gate))).astype(BF16)


def update(qkvg, cosine, sine, gain, gamma, state):
    whole = lambda shape: pl.BlockSpec(shape, lambda i: (0,) * len(shape))
    block = pl.BlockSpec((STEP, LH, HD, HD), lambda i: (i, 0, 0, 0))
    return pl.pallas_call(
        state_kernel,
        grid=(T // STEP,),
        out_shape=(
            jax.ShapeDtypeStruct((T, RW), BF16),
            jax.ShapeDtypeStruct((T, LH, HD, HD), F32),
        ),
        in_specs=[
            whole((T, 4 * RW)), whole((T, HD)), whole((T, HD)), whole((1, RW)), SM, block,
        ],
        out_specs=(whole((T, RW)), block),
        scratch_shapes=[
            pltpu.VMEM((T, 16, HD), F32),
            pltpu.VMEM((T, 8, HD), F32),
            pltpu.VMEM((T, 8, HD), F32),
        ],
        name="state",
    )(qkvg, cosine, sine, gain, gamma, state)


def silu(x):
    return x * jax.nn.sigmoid(x)


def ffn_kernel(
    ret_ref, x_ref, gain_ref, bg_ref, sel_ref, wo_in, dw_in, eg_in, eu_in, ed_in,
    out_ref,
    wo, dgt, dut, ddn, eg, eu, ed,
    retz, mo, mx, nf, xp, selg, seb, ein, eo, eop, er, rin, dp, dpp, po, rsl, lo,
    send, recv, local,
):
    at = Links(send, recv, local)
    z, p, c = at.z, at.p, at.c
    o = 1 - c
    me = at.chip(z, p)
    bar, greeted = at.barrier_signal(True)
    wo_copy = at.pull(wo_in, wo)
    e_copies = [at.pull(a, b) for a, b in ((eg_in, eg), (eu_in, eu), (ed_in, ed))]
    d_copies = [at.pull(dw_in.at[:, j], w) for j, w in enumerate((dgt, dut, ddn))]
    retz[z] = ret_ref[...]
    selg[0] = sel_ref[0]
    pl.semaphore_wait(bar, greeted)
    sends = []

    def push(*args):
        copy = at.push(*args)
        sends.append(copy)
        return copy

    ret_copies = [push(ret_ref, retz.at[z], at.chip((z + k) % NZ, p), c) for k in range(1, NZ)]
    sel_copies = [push(sel_ref.at[d], selg.at[d], at.chip(z, at.plane(d)), c) for d in range(1, NP)]
    wo_copy.wait()
    for copy in ret_copies:
        copy.wait_recv()
    mixed = lax.dot_general(
        retz[...].reshape(NZ * T, RW), wo[...].reshape(512, RW), NT, preferred_element_type=F32
    )
    mo[...] = mixed.astype(BF16).reshape(NZ, T, 512)
    mx[c, z] = mo[z]
    mx_copies = [push(mo.at[z], mx.at[c, z], me, o)]
    for k in range(1, NZ):
        to = (z + k) % NZ
        for core in (c, o):
            mx_copies.append(push(mo.at[to], mx.at[c, z], at.chip(to, p), core))
    for copy in mx_copies:
        copy.wait_recv()
    mixer = [(mx[0, k].astype(F32) + mx[1, k].astype(F32)).astype(BF16) for k in range(NZ)]
    mixer_out = jnp.concatenate(mixer, axis=-1).astype(F32)
    residual = (x_ref[...].astype(F32) + mixer_out).astype(BF16)
    normed = rms(residual.astype(F32), gain_ref[...])
    for h in range(2):
        nf[h] = normed[:, h * 1024 : (h + 1) * 1024]
        xp[h, 0] = normed[:, h * 1024 : (h + 1) * 1024]
        lo[h] = residual[:, h * 1024 : (h + 1) * 1024]

    x_copies = [
        push(nf.at[c], xp.at[c, d], at.chip(z, at.plane(d)), c) for d in range(1, NP)
    ]
    for copy in sel_copies:
        copy.wait_recv()
    weights = selg[...].reshape(NP * T, 128)
    w_hi = weights.astype(BF16)
    w_lo = (weights - w_hi.astype(F32)).astype(BF16)
    chosen = jnp.where(weights.T > 0.0, 1.0, 0.0).astype(BF16)
    f_copies = []
    for d in range(1, NP):
        x_copies[d - 1].wait_recv()
        f_copies.append(push(xp.at[c, d], xp.at[c, d], me, o))
    picked = jnp.dot(chosen, xp[c].reshape(NP * T, 1024), preferred_element_type=F32)
    seb[...] = picked.astype(BF16).reshape(NZ, 32, 1024)
    ein[c, z] = seb[z]
    e_out = [
        push(seb.at[(z + k) % NZ], ein.at[c, z], at.chip((z + k) % NZ, p), c) for k in range(1, NZ)
    ]
    e_pair = [push(seb.at[z], ein.at[c, z], me, o)]

    for copy in d_copies:
        copy.wait()
    for copy in f_copies:
        copy.wait_recv()
    gate = jnp.zeros((NP * T, 128), F32)
    up = jnp.zeros((NP * T, 128), F32)
    opening = jnp.zeros((NP * T, 1), F32)
    for h in range(2):
        cols = slice(h * 1024, (h + 1) * 1024)
        block = xp[h].reshape(NP * T, 1024)
        gate = gate + lax.dot_general(
            block, dgt[:, :, cols].reshape(128, 1024), NT, preferred_element_type=F32
        )
        up = up + lax.dot_general(
            block, dut[:, :, cols].reshape(128, 1024), NT, preferred_element_type=F32
        )
        opening = opening + jnp.sum(
            block.astype(F32) * bg_ref[:, cols].astype(F32), axis=-1, keepdims=True
        )
    opening = jax.nn.sigmoid(opening)
    hidden = (silu(gate) * up).astype(BF16)
    down = ddn[...].reshape(128, D)
    for h in range(2):
        term = jnp.dot(
            hidden, down[:, h * 1024 : (h + 1) * 1024], preferred_element_type=F32
        )
        dp[h] = (term * opening).astype(BF16)
    dp_copy = push(dp.at[o], dpp, me, o)

    for k in range(1, NZ):
        e_out[k - 1].wait_recv()
        frm = (z + NZ - k) % NZ
        e_pair.append(push(ein.at[c, frm], ein.at[c, frm], me, o))
    for copy in e_copies:
        copy.wait()
    for copy in e_pair:
        copy.wait_recv()
    gate = jnp.zeros((128, 512), F32)
    up = jnp.zeros((128, 512), F32)
    for h in range(2):
        block = ein[h].reshape(128, 1024)
        rows = slice(h * 1024, (h + 1) * 1024)
        gate = gate + jnp.dot(block, eg[rows, :], preferred_element_type=F32)
        up = up + jnp.dot(block, eu[rows, :], preferred_element_type=F32)
    hidden = (silu(gate) * up).astype(BF16)
    for h in range(2):
        eo[h] = jnp.dot(
            hidden, ed[:, h * 1024 : (h + 1) * 1024], preferred_element_type=F32
        ).astype(BF16)
    eo_copy = push(eo.at[o], eop, me, o)
    eo_copy.wait_recv()
    er[...] = (eo[c].astype(F32) + eop[...].astype(F32)).astype(BF16).reshape(NZ, 32, 1024)
    rin[z] = er[z]
    r_copies = [
        push(er.at[(z + k) % NZ], rin.at[z], at.chip((z + k) % NZ, p), c) for k in range(1, NZ)
    ]
    dp_copy.wait_recv()
    for copy in r_copies:
        copy.wait_recv()
    results = rin[...].reshape(128, 1024)
    total = jnp.dot(w_hi, results, preferred_element_type=F32)
    total = total + jnp.dot(w_lo, results, preferred_element_type=F32)
    total = total + (dp[c].astype(F32) + dpp[...].astype(F32))
    po[...] = total.astype(BF16).reshape(NP, T, 1024)
    s_copies = []
    for d in range(1, NP):
        back = (((at.y + 4 - d // 4) % 4) * 4) + (at.x + 4 - d % 4) % 4
        s_copies.append(push(po.at[d], rsl.at[d], at.chip(z, back), c))
    total = po[0].astype(F32)
    for d in range(1, NP):
        s_copies[d - 1].wait_recv()
        total = total + rsl[d].astype(F32)
    nf_out = (lo[c].astype(F32) + total).astype(BF16)
    lo[2] = nf_out
    l_copy = push(lo.at[2], lo.at[3], me, o)
    l_copy.wait_recv()
    mine, other = nf_out, lo[3]
    first = jnp.where(c == 0, mine, other)
    second = jnp.where(c == 0, other, mine)
    out_ref[:, :1024] = first
    out_ref[:, 1024:] = second
    for copy in sends:
        copy.wait_send()


def ffn(ret, x, gain, bg, sel, wo, dw, eg, eu, ed):
    v = lambda shape, dtype=BF16: pltpu.VMEM(shape, dtype)
    return pl.pallas_call(
        ffn_kernel,
        out_shape=jax.ShapeDtypeStruct((T, D), BF16),
        in_specs=[VM] * 5 + [ANY] * 5,
        out_specs=VM,
        scratch_shapes=[
            v((NP, 32, RW)),
            v((NZ, 32, D)), v((NZ, 32, D)), v((NZ, 32, D)),
            v((D, 512)), v((D, 512)), v((512, D)),
            v((NZ, T, RW)), v((NZ, T, 512)), v((2, NZ, T, 512)),
            v((2, T, 1024)), v((2, NP, T, 1024)), v((NP, T, 128), F32),
            v((NZ, 32, 1024)), v((2, NZ, 32, 1024)), v((2, 128, 1024)), v((128, 1024)),
            v((NZ, 32, 1024)), v((NZ, 32, 1024)),
            v((2, NP * T, 1024)), v((NP * T, 1024)),
            v((NP, T, 1024)), v((NP, T, 1024)), v((4, T, 1024)),
            pltpu.SemaphoreType.DMA((96,)),
            pltpu.SemaphoreType.DMA((96,)),
            pltpu.SemaphoreType.DMA((12,)),
        ],
        compiler_params=pltpu.CompilerParams(
            collective_id=1, has_side_effects=True, vmem_limit_bytes=60 * 1024 * 1024
        ),
        name="ffn",
    )(ret, x, gain, bg, sel, wo, dw, eg, eu, ed)


def selection(route_ids, route_weight):
    p = lax.axis_index("ep") % NP
    y, x = p // 4, p % 4
    flat = route_ids.reshape(-1)
    count = flat.shape[0]
    earlier = jnp.arange(count)[None, :] < jnp.arange(count)[:, None]
    slot = jnp.sum(((flat[:, None] == flat[None, :]) & earlier).astype(jnp.int32), axis=1)
    slot = slot.reshape(route_ids.shape)
    to_z, to_p = route_ids // NP, route_ids % NP
    shift = ((to_p // 4 + 4 - y) % 4) * 4 + (to_p % 4 + 4 - x) % 4
    lane = to_z * 32 + 2 * shift + slot
    widened = route_weight.astype(F32)
    share = widened / jnp.sum(widened, axis=-1, keepdims=True)
    lanes = jnp.arange(128, dtype=jnp.int32)
    shifts = jnp.arange(NP, dtype=jnp.int32)
    total = jnp.zeros((NP, T, 128), F32)
    for k in range(route_ids.shape[1]):
        hit = (shift[None, :, k, None] == shifts[:, None, None]) & (
            lane[None, :, k, None] == lanes[None, None, :]
        )
        total = total + jnp.where(hit, share[None, :, k, None], 0.0)
    return total


def log_decay(head_count):
    spread = jnp.arange(head_count, dtype=F32) * (5.0 / max(head_count - 1, 1))
    return jnp.log1p(-(2.0 ** (-5.0 - spread)))


def on_device(
    inputs, positions, ret_state, norm_mix, w_query, w_key, w_value, w_gate_in, head_gain, w_out,
    norm_ffn, route_ids, route_weight, exp_gate, exp_up, exp_down, dense_gate, dense_up,
    dense_down, branch_gate,
):
    qkvg, wo, dw = project(
        inputs, norm_mix[None, :], w_query, w_key, w_value, w_gate_in,
        w_out.T, dense_gate.T, dense_up.T, dense_down,
    )
    frequency = 10000.0 ** (-jnp.arange(HD // 2, dtype=F32) * 2.0 / HD)
    angles = positions.astype(F32)[:, None] * frequency[None, :]
    cosine, sine = jnp.cos(angles), jnp.sin(angles)
    gamma = lax.dynamic_slice_in_dim(
        jnp.exp(log_decay(HEADS)), lax.axis_index("tp") * LH, LH
    )
    ret, new_state = update(
        qkvg,
        jnp.concatenate([cosine, cosine], axis=-1),
        jnp.concatenate([-sine, sine], axis=-1),
        head_gain[None, :],
        gamma,
        ret_state,
    )
    layer_out = ffn(
        ret, inputs, norm_ffn[None, :], branch_gate[None, :], selection(route_ids, route_weight),
        wo, dw, exp_gate[0], exp_up[0], exp_down[0],
    )
    return (layer_out, new_state)


def solution(mesh):
    in_specs = (
        P("ep", None),
        P("ep"),
        P("ep", "tp", None, None),
        P(),
        P("ep", "tp"),
        P("ep", "tp"),
        P("ep", "tp"),
        P("ep", "tp"),
        P("tp"),
        P("tp", "ep"),
        P(),
        P("ep", None),
        P("ep", None),
        P("ep", None, "tp"),
        P("ep", None, "tp"),
        P("ep", "tp", None),
        P(None, ("ep", "tp")),
        P(None, ("ep", "tp")),
        P(("ep", "tp"), None),
        P(),
    )
    out_specs = (P("ep", None), P("ep", "tp", None, None))
    return jax.shard_map(
        on_device, mesh=mesh, in_specs=in_specs, out_specs=out_specs, check_vma=False
    )
```
